32 devices in a mesh: fs: 16 (over z, y, x), tp: 2 (over core).
Axes of the slice: x: 2, y: 2, z: 4, core: 2. Of those that a mesh axis runs over, the one named last changes fastest.
Arguments:
- tokens: bfloat16 [6144, 2048], P('fs', 'tp'), may hold values from -24 to 24
- mixer_gain: float32 [2048], replicated, may hold values from 0.1 to 1.9
- pool_input: bfloat16 [2048, 1024], P('fs', 'tp'), may hold values from -0.125 to 0.125
- group_weight: bfloat16 [8, 128, 128], P('tp'), may hold values from -0.5 to 0.5
- channel_scale: float32 [1024], P('tp'), may hold values from 0.5 to 2
- pool_output: bfloat16 [1024, 2048], P('tp', 'fs'), may hold values from -0.1875 to 0.1875
- ffn_gain: float32 [2048], replicated, may hold values from 0.1 to 1.9
- gate_weight: bfloat16 [2048, 5632], P('fs', 'tp'), may hold values from -0.125 to 0.125
- up_weight: bfloat16 [2048, 5632], P('fs', 'tp'), may hold values from -0.125 to 0.125
- down_weight: bfloat16 [5632, 2048], P('tp', 'fs'), may hold values from -0.078125 to 0.078125
- final_gain: float32 [2048], P('tp'), may hold values from 0.1 to 1.9
Outputs:
- normed_out: bfloat16 [6144, 2048], P('fs', 'tp')
The draws below stay inside these ranges and needn't reach their ends.
All inputs are finite; a program needn't handle non-finite values.
Results may differ from the reference program's by a relative error of at most 0.015.
Values may be sent and summed in bfloat16 or wider, within the bound.
No kernel may reach another device: no remote copies, remote signals or barrier semaphores. Data moves between devices by JAX's collectives and lax.ppermute only.
A program may use at most 128 MiB of HBM per device.

```python
import math
import jax
import jax.numpy as jnp
from jax import lax

D = 2048
FF = 5632
GROUPS = 8
GROUP_DIM = 128
POOL = 1024
LENGTH = 128
TOKENS = 6144
N_TP = 2


def draw_tokens(key, part):
    base_key, column_key = jax.random.split(jax.random.fold_in(key, 11), 2)
    values = jax.random.normal(base_key, (TOKENS, D), jnp.float32)
    column_scales = jnp.exp(jax.random.uniform(column_key, (8,), jnp.float32, jnp.log(0.3), jnp.log(3.0)))
    values = values * jnp.repeat(column_scales, D // 8)[None, :]
    return jnp.clip(values, -24.0, 24.0).astype(jnp.bfloat16)


def level_of(rng, extent, cuts, least, high):
    level, own = 1.0, jax.random.fold_in(rng, 6)
    for axis_at, parts in cuts:
        heights = jnp.exp(jax.random.uniform(jax.random.fold_in(own, axis_at), (parts,), jnp.float32, least / len(cuts), high / len(cuts)))
        level = level * jnp.repeat(heights, extent[axis_at] // parts).reshape([-1 if axis == axis_at else 1 for axis in range(len(extent))])
    return level


def normal_values(rng, extent, scale, reach, cuts=(), kind=jnp.bfloat16):
    level = level_of(rng, extent, cuts, -0.22, 0.18) if cuts else 1.0
    array = jax.random.normal(rng, extent, jnp.float32) * scale * level
    return jnp.minimum(jnp.maximum(array, -reach), reach).astype(kind)


def setup_inputs(seed: int = 0) -> dict:
    keys = jax.random.split(jax.random.key(seed), 12)
    tokens = draw_tokens(jax.random.fold_in(keys[11], 71), 0)
    mixer_gain = jnp.clip(1.0 + 0.18 * jax.random.normal(keys[1], (D,), jnp.float32), 0.1, 1.9)
    pool_input = normal_values(keys[2], (D, POOL), D ** -0.5, 0.125, ((0, 16), (1, 2)))
    group_weight = normal_values(keys[3], (GROUPS, GROUP_DIM, GROUP_DIM), GROUP_DIM ** -0.5, 0.5, ((0, 2),))
    channel_scale = jnp.clip(jnp.exp(math.log(2.0) - 1.3862944 * jax.random.uniform(keys[4], (POOL,), jnp.float32) ** level_of(keys[4], (POOL,), ((0, 2),), -0.2, 0.2)), 0.5, 2.0)
    pool_output = normal_values(keys[5], (POOL, D), POOL ** -0.5, 0.1875, ((0, 2), (1, 16)))
    ffn_gain = jnp.clip(1.0 + 0.18 * jax.random.normal(keys[6], (D,), jnp.float32), 0.1, 1.9)
    gate_weight = normal_values(keys[7], (D, FF), D ** -0.5, 0.125, ((0, 16), (1, 2)))
    up_weight = normal_values(keys[8], (D, FF), D ** -0.5, 0.125, ((0, 16), (1, 2)))
    down_weight = normal_values(keys[9], (FF, D), FF ** -0.5, 0.078125, ((0, 2), (1, 16)))
    final_gain = jnp.clip(1.0 + 0.18 * jax.random.normal(keys[10], (D,), jnp.float32), 0.1, 1.9)
    return dict(tokens=tokens, mixer_gain=mixer_gain, pool_input=pool_input, group_weight=group_weight, channel_scale=channel_scale, pool_output=pool_output, ffn_gain=ffn_gain, gate_weight=gate_weight, up_weight=up_weight, down_weight=down_weight, final_gain=final_gain)


EPS = 1e-06

def rms(values, gain):
    wide = values.astype(jnp.float32)
    scaled = wide * jax.lax.rsqrt(lax.optimization_barrier(jnp.mean(wide * wide, axis=-1, keepdims=True)) + EPS)
    return scaled * gain.astype(jnp.float32)

def blocked_product(left, right, blocks):
    width = left.shape[1] // blocks
    total = jnp.zeros((left.shape[0], right.shape[1]), jnp.float32)
    for block in range(blocks):
        part = jnp.dot(left[:, block * width:(block + 1) * width], right[block * width:(block + 1) * width], preferred_element_type=jnp.float32)
        total = total + part.astype(jnp.bfloat16).astype(jnp.float32)
    return total

def reference(tokens, mixer_gain, pool_input, group_weight, channel_scale, pool_output, ffn_gain, gate_weight, up_weight, down_weight, final_gain):
    count_rows = tokens.shape[0]
    first_normed = rms(tokens, mixer_gain).astype(jnp.bfloat16)
    pooled_in = jnp.dot(first_normed, pool_input, preferred_element_type=jnp.float32).astype(jnp.bfloat16)
    grid = pooled_in.astype(jnp.float32).reshape(count_rows // LENGTH, LENGTH, GROUPS, GROUP_DIM)
    prefix = jnp.cumsum(grid, axis=1)
    counts = jnp.arange(1, LENGTH + 1, dtype=jnp.float32)[None, :, None]
    pieces = []
    for group in range(GROUPS):
        window = 2 ** (1 + group % 4)
        running = prefix[:, :, group]
        lagged = jnp.pad(running, ((0, 0), (window, 0), (0, 0)))[:, :LENGTH]
        average = (running - lagged) / jnp.minimum(counts, float(window))
        pieces.append(average - grid[:, :, group])
    pooled = jnp.stack(pieces, axis=2).astype(jnp.bfloat16).reshape(count_rows, GROUPS, GROUP_DIM)
    mapped = jnp.einsum('ngc,gcd->ngd', pooled.astype(jnp.float32), group_weight.astype(jnp.float32))
    grouped = (mapped.reshape(count_rows, GROUPS * GROUP_DIM) * channel_scale).astype(jnp.bfloat16)
    mixer_out = blocked_product(grouped, pool_output, N_TP)
    middle = (tokens.astype(jnp.float32) + mixer_out).astype(jnp.bfloat16)
    second_normed = rms(middle, ffn_gain).astype(jnp.bfloat16)
    gate = jnp.dot(second_normed, gate_weight, preferred_element_type=jnp.float32)
    upward = jnp.dot(second_normed, up_weight, preferred_element_type=jnp.float32)
    hidden = (jax.nn.silu(gate) * upward).astype(jnp.bfloat16)
    ffn_out = blocked_product(hidden, down_weight, N_TP)
    closing = middle.astype(jnp.float32) + ffn_out
    return rms(closing, final_gain).astype(jnp.bfloat16)
```

```python
import jax
import jax.numpy as jnp
from jax import lax
from jax.sharding import PartitionSpec as P

GROUP_DIM = 128
LENGTH = 128
EPS = 1e-06
SHARE_BITS = (0, 2)


def rms(values, gain):
    wide = values.astype(jnp.float32)
    scaled = wide * lax.rsqrt(jnp.mean(wide * wide, axis=-1, keepdims=True) + EPS)
    return scaled * gain


def dot(left, right):
    return jnp.dot(left, right, preferred_element_type=jnp.float32)


def dot_t(left, right):
    return lax.dot_general(
        left, right, (((1,), (1,)), ((), ())), preferred_element_type=jnp.float32
    )


def flip(value, mask):
    count = lax.axis_size("fs")
    return lax.ppermute(value, "fs", [(i, i ^ mask) for i in range(count)])


def bit_of(index, bit):
    return jnp.bitwise_and(jnp.right_shift(index, bit), 1)


def mask_of(bits, number):
    return sum(((number >> at) & 1) << bit for at, bit in enumerate(bits))


def spread(weight, shared, order):
    count = lax.axis_size("fs")
    bits = count.bit_length() - 1
    me = lax.axis_index("fs")
    rows, columns = weight.shape
    parts = 1 << len(shared)
    width = columns // parts
    zero = jnp.int32(0)
    if parts > 1:
        blocks = jnp.transpose(weight.reshape(rows, parts, width), (1, 0, 2))
        mine = sum(jnp.left_shift(bit_of(me, bit), at) for at, bit in enumerate(shared))
        held = jnp.zeros((parts, rows, width), weight.dtype)
        for number in reversed(range(parts)):
            peer = jnp.bitwise_xor(mine, number)
            block = lax.dynamic_slice(blocks, (peer, zero, zero), (1, rows, width))
            if number:
                block = flip(block, mask_of(shared, number))
            held = lax.dynamic_update_slice(held, block, (peer, zero, zero))
    else:
        held = weight.reshape(1, rows, width)
    pieces = {0: held}
    for bit in order:
        for key in list(pieces):
            pieces[key | (1 << bit)] = flip(pieces[key], 1 << bit)
    axes = list(reversed(range(bits)))
    whole = jnp.zeros((2,) * bits + (rows, width), weight.dtype)
    small = tuple(2 if bit in shared else 1 for bit in axes) + (rows, width)
    for key, piece in pieces.items():
        start = tuple(
            zero if bit in shared else bit_of(jnp.bitwise_xor(me, key), bit) for bit in axes
        ) + (zero, zero)
        whole = lax.dynamic_update_slice(whole, piece.reshape(small), start)
    return whole.reshape(count * rows, width)


def join_columns(own):
    if lax.axis_size("tp") != 2:
        return lax.all_gather(own, "tp", axis=1, tiled=True)
    other = lax.ppermute(own, "tp", [(0, 1), (1, 0)])
    first = lax.axis_index("tp") == 0
    return jnp.concatenate(
        [jnp.where(first, own, other), jnp.where(first, other, own)], axis=1
    )


def halves(weight_t):
    size = weight_t.shape[0] // 2
    mine = lax.axis_index("tp")
    return (
        lax.dynamic_slice_in_dim(weight_t, mine * size, size, 0),
        lax.dynamic_slice_in_dim(weight_t, (1 - mine) * size, size, 0),
    )


def sum_columns(left, weight_t, cut):
    if cut is None:
        terms = dot_t(left, weight_t).astype(jnp.bfloat16)
        return lax.psum_scatter(terms, "tp", scatter_dimension=1, tiled=True).astype(jnp.float32)
    keep, give = cut
    given = lax.ppermute(dot_t(left, give).astype(jnp.bfloat16), "tp", [(0, 1), (1, 0)])
    kept = dot_t(left, keep).astype(jnp.bfloat16)
    return kept.astype(jnp.float32) + given.astype(jnp.float32)


def local(
    tokens,
    mixer_gain,
    pool_input,
    group_weight,
    channel_scale,
    pool_output,
    ffn_gain,
    gate_weight,
    up_weight,
    down_weight,
    final_gain,
):
    count = lax.axis_size("fs")
    bits = count.bit_length() - 1
    pair = lax.axis_size("tp") == 2
    shared = tuple(bit for bit in SHARE_BITS if bit < bits)
    rest = tuple(bit for bit in reversed(range(bits)) if bit not in shared)
    high = tuple(bit for bit in reversed(range(2, bits)))
    width = tokens.shape[1] * lax.axis_size("tp")

    pool_in = spread(pool_input, (), high + tuple(b for b in (0, 1) if b < bits))
    pool_out_t = spread(pool_output.T, (), high + tuple(b for b in (1, 0) if b < bits))
    gate_all = spread(gate_weight, shared, rest)
    up_all = spread(up_weight, shared, rest)
    down_t = spread(down_weight.T, shared, rest)

    first_normed = rms(join_columns(tokens), mixer_gain).astype(jnp.bfloat16)
    row_count = first_normed.shape[0]
    pooled_in = dot(first_normed, pool_in).astype(jnp.bfloat16)
    local_groups = group_weight.shape[0]
    group_ids = lax.axis_index("tp") * local_groups + jnp.arange(local_groups, dtype=jnp.int32)
    windows = jnp.left_shift(jnp.int32(2), group_ids % 4)
    later = jnp.arange(LENGTH, dtype=jnp.int32)[None, :, None]
    earlier = jnp.arange(LENGTH, dtype=jnp.int32)[None, None, :]
    reach = windows[:, None, None]
    inside = (earlier <= later) & (earlier > later - reach)
    band = inside.astype(jnp.bfloat16)
    divisor = jnp.minimum(later[:, :, 0] + 1, windows[:, None]).astype(jnp.float32)
    grid_low = pooled_in.reshape(row_count // LENGTH, LENGTH, local_groups, GROUP_DIM)
    window_sums = jnp.einsum("gts,nsgc->ntgc", band, grid_low, preferred_element_type=jnp.float32)
    average = window_sums / jnp.transpose(divisor)[None, :, :, None]
    pooled = (
        (average - grid_low.astype(jnp.float32))
        .astype(jnp.bfloat16)
        .reshape(row_count, local_groups, GROUP_DIM)
    )
    mapped = jnp.einsum("ngc,gcd->ngd", pooled, group_weight, preferred_element_type=jnp.float32)
    grouped = (mapped.reshape(row_count, local_groups * GROUP_DIM) * channel_scale).astype(
        jnp.bfloat16
    )
    mixer_out = sum_columns(grouped, pool_out_t, halves(pool_out_t) if pair else None)
    middle = (tokens.astype(jnp.float32) + mixer_out).astype(jnp.bfloat16)

    down_cut = halves(down_t) if pair else None
    masks = [mask_of(shared, number) for number in range(1 << len(shared))]
    arrived = [flip(middle, mask) if mask else middle for mask in masks]
    ffn_out = None
    for mask, part in reversed(list(zip(masks, arrived))):
        normed = rms(join_columns(part), ffn_gain).astype(jnp.bfloat16)
        gate = dot(normed, gate_all)
        upward = dot(normed, up_all)
        hidden = (jax.nn.silu(gate) * upward).astype(jnp.bfloat16)
        terms = sum_columns(hidden, down_t, down_cut)
        if mask:
            terms = flip(terms.astype(jnp.bfloat16), mask).astype(jnp.float32)
        ffn_out = terms if ffn_out is None else ffn_out + terms

    closing = middle.astype(jnp.float32) + ffn_out
    squares = lax.psum(jnp.sum(closing * closing, axis=1, keepdims=True), "tp")
    scaled = closing * lax.rsqrt(squares / width + EPS) * final_gain
    return scaled.astype(jnp.bfloat16)


def solution(mesh):
    placed = (
        P("fs", "tp"),
        P(),
        P("fs", "tp"),
        P("tp", None, None),
        P("tp"),
        P("tp", "fs"),
        P(),
        P("fs", "tp"),
        P("fs", "tp"),
        P("tp", "fs"),
        P("tp"),
    )
    return jax.shard_map(
        local, mesh=mesh, in_specs=placed, out_specs=P("fs", "tp"), check_vma=False
    )
```

```python
import jax
import jax.numpy as jnp
from jax import lax
from jax.experimental.layout import Layout, with_layout_constraint
from jax.sharding import PartitionSpec as P

GROUP_DIM = 128
LENGTH = 128
EPS = 1e-06
SHARE_BITS = (0, 2)


def rms(values, gain):
    wide = values.astype(jnp.float32)
    scaled = wide * lax.rsqrt(jnp.mean(wide * wide, axis=-1, keepdims=True) + EPS)
    return scaled * gain


def dot(left, right):
    return jnp.dot(left, right, preferred_element_type=jnp.float32)


def dot_t(left, right):
    return lax.dot_general(
        left, right, (((1,), (1,)), ((), ())), preferred_element_type=jnp.float32
    )


def flip(value, mask):
    count = lax.axis_size("fs")
    return lax.ppermute(value, "fs", [(i, i ^ mask) for i in range(count)])


def bit_of(index, bit):
    return jnp.bitwise_and(jnp.right_shift(index, bit), 1)


def mask_of(bits, number):
    return sum(((number >> at) & 1) << bit for at, bit in enumerate(bits))


def rowwise(value):
    return with_layout_constraint(value, Layout(tuple(range(value.ndim))))


def spread(weight, shared, stages):
    count = lax.axis_size("fs")
    bits = count.bit_length() - 1
    axes = list(reversed(range(bits)))
    me = lax.axis_index("fs")
    rows, columns = weight.shape
    parts = 1 << len(shared)
    width = columns // parts
    zero = jnp.int32(0)

    def shape_of(have):
        return tuple(2 if bit in have else 1 for bit in axes) + (rows, width)

    def assemble(pieces, have, added):
        whole = rowwise(jnp.zeros(shape_of(have + added), weight.dtype))
        for key, piece in pieces.items():
            start = tuple(
                bit_of(jnp.bitwise_xor(me, key), bit) if bit in added else zero for bit in axes
            ) + (zero, zero)
            whole = lax.dynamic_update_slice(whole, piece.reshape(shape_of(have)), start)
        return rowwise(whole)

    if parts > 1:
        blocks = rowwise(jnp.transpose(weight.reshape(rows, parts, width), (1, 0, 2)))
        mine = sum(jnp.left_shift(bit_of(me, bit), at) for at, bit in enumerate(shared))
        pieces = {}
        for number in range(parts):
            peer = jnp.bitwise_xor(mine, number)
            block = lax.dynamic_slice(blocks, (peer, zero, zero), (1, rows, width))
            mask = mask_of(shared, number)
            pieces[mask] = rowwise(flip(block, mask) if mask else block)
        held, have = assemble(pieces, (), shared), shared
    else:
        held, have = rowwise(weight), ()
    for stage in stages:
        pieces = {0: held}
        for bit in stage:
            for key in list(pieces):
                pieces[key | (1 << bit)] = rowwise(flip(pieces[key], 1 << bit))
        held, have = assemble(pieces, have, stage), have + stage
    return rowwise(held.reshape(count * rows, width))


def join_columns(own):
    if lax.axis_size("tp") != 2:
        return lax.all_gather(own, "tp", axis=1, tiled=True)
    other = lax.ppermute(own, "tp", [(0, 1), (1, 0)])
    first = lax.axis_index("tp") == 0
    return jnp.concatenate(
        [jnp.where(first, own, other), jnp.where(first, other, own)], axis=1
    )


def halves(weight_t):
    size = weight_t.shape[0] // 2
    mine = lax.axis_index("tp")
    return (
        lax.dynamic_slice_in_dim(weight_t, mine * size, size, 0),
        lax.dynamic_slice_in_dim(weight_t, (1 - mine) * size, size, 0),
    )


def sum_columns(left, weight_t, cut):
    if cut is None:
        terms = dot_t(left, weight_t).astype(jnp.bfloat16)
        return lax.psum_scatter(terms, "tp", scatter_dimension=1, tiled=True).astype(jnp.float32)
    keep, give = cut
    given = lax.ppermute(dot_t(left, give).astype(jnp.bfloat16), "tp", [(0, 1), (1, 0)])
    kept = dot_t(left, keep).astype(jnp.bfloat16)
    return kept.astype(jnp.float32) + given.astype(jnp.float32)


def local(
    tokens,
    mixer_gain,
    pool_input,
    group_weight,
    channel_scale,
    pool_output,
    ffn_gain,
    gate_weight,
    up_weight,
    down_weight,
    final_gain,
):
    count = lax.axis_size("fs")
    bits = count.bit_length() - 1
    pair = lax.axis_size("tp") == 2
    shared = tuple(bit for bit in SHARE_BITS if bit < bits)
    rest = tuple(bit for bit in reversed(range(bits)) if bit not in shared)
    high = tuple(bit for bit in reversed(range(2, bits)))
    width = tokens.shape[1] * lax.axis_size("tp")

    low = tuple(bit for bit in (0, 1) if bit < bits)
    pool_in = spread(pool_input, (), (high, low))
    pool_out_t = spread(pool_output.T, (), (high, low[::-1]))
    gate_all = spread(gate_weight, shared, (rest,))
    up_all = spread(up_weight, shared, (rest,))
    down_t = spread(down_weight.T, shared, (rest,))

    first_normed = rms(join_columns(tokens), mixer_gain).astype(jnp.bfloat16)
    row_count = first_normed.shape[0]
    pooled_in = dot(first_normed, pool_in).astype(jnp.bfloat16)
    local_groups = group_weight.shape[0]
    group_ids = lax.axis_index("tp") * local_groups + jnp.arange(local_groups, dtype=jnp.int32)
    windows = jnp.left_shift(jnp.int32(2), group_ids % 4)
    later = jnp.arange(LENGTH, dtype=jnp.int32)[None, :, None]
    earlier = jnp.arange(LENGTH, dtype=jnp.int32)[None, None, :]
    reach = windows[:, None, None]
    inside = (earlier <= later) & (earlier > later - reach)
    band = inside.astype(jnp.bfloat16)
    divisor = jnp.minimum(later[:, :, 0] + 1, windows[:, None]).astype(jnp.float32)
    grid_low = pooled_in.reshape(row_count // LENGTH, LENGTH, local_groups, GROUP_DIM)
    window_sums = jnp.einsum("gts,nsgc->ntgc", band, grid_low, preferred_element_type=jnp.float32)
    average = window_sums / jnp.transpose(divisor)[None, :, :, None]
    pooled = (
        (average - grid_low.astype(jnp.float32))
        .astype(jnp.bfloat16)
        .reshape(row_count, local_groups, GROUP_DIM)
    )
    mapped = jnp.einsum("ngc,gcd->ngd", pooled, group_weight, preferred_element_type=jnp.float32)
    grouped = (mapped.reshape(row_count, local_groups * GROUP_DIM) * channel_scale).astype(
        jnp.bfloat16
    )
    mixer_out = sum_columns(grouped, pool_out_t, halves(pool_out_t) if pair else None)
    middle = (tokens.astype(jnp.float32) + mixer_out).astype(jnp.bfloat16)

    down_cut = halves(down_t) if pair else None
    masks = [mask_of(shared, number) for number in range(1 << len(shared))]
    arrived = [flip(middle, mask) if mask else middle for mask in masks]
    ffn_out = None
    for mask, part in reversed(list(zip(masks, arrived))):
        normed = rms(join_columns(part), ffn_gain).astype(jnp.bfloat16)
        gate = dot(normed, gate_all)
        upward = dot(normed, up_all)
        hidden = (jax.nn.silu(gate) * upward).astype(jnp.bfloat16)
        terms = sum_columns(hidden, down_t, down_cut)
        if mask:
            terms = flip(terms.astype(jnp.bfloat16), mask).astype(jnp.float32)
        ffn_out = terms if ffn_out is None else ffn_out + terms

    closing = middle.astype(jnp.float32) + ffn_out
    squares = lax.psum(jnp.sum(closing * closing, axis=1, keepdims=True), "tp")
    scaled = closing * lax.rsqrt(squares / width + EPS) * final_gain
    return scaled.astype(jnp.bfloat16)


def solution(mesh):
    placed = (
        P("fs", "tp"),
        P(),
        P("fs", "tp"),
        P("tp", None, None),
        P("tp"),
        P("tp", "fs"),
        P(),
        P("fs", "tp"),
        P("fs", "tp"),
        P("tp", "fs"),
        P("tp"),
    )
    return jax.shard_map(
        local, mesh=mesh, in_specs=placed, out_specs=P("fs", "tp"), check_vma=False
    )
```
